32 devices in a mesh: grp: 2 (over y), sp: 4 (over z), tp: 4 (over x, core).
Axes of the slice: x: 2, y: 2, z: 4, core: 2. Of those that a mesh axis runs over, the one named last changes fastest.
Arguments:
- tokens: bfloat16 [4096, 2, 2048], P(('grp', 'sp', 'tp')), parts along dimension 0, may hold values from -64 to 64
- w_query: bfloat16 [2048, 2048], P(None, 'tp'), may hold values from -0.21875 to 0.21875
- w_key: bfloat16 [2048, 2048], P(None, 'tp'), may hold values from -0.125 to 0.125
- w_value: bfloat16 [2048, 2048], P(None, 'tp'), may hold values from -0.125 to 0.125
- w_out: bfloat16 [2048, 2048], P('tp'), may hold values from -0.125 to 0.125
- head_lambda: float32 [16], P('tp'), may hold values from 0.3 to 0.8
- sub_gain: float32 [128], replicated, may hold values from 0.1 to 1.9
Outputs:
- mixed: bfloat16 [4096, 2, 2048], P(('grp', 'sp', 'tp')), parts along dimension 0
The draws below stay inside these ranges and needn't reach their ends.
There are 2 independent parts, one for each index of `grp`. The reference program is written for one: setup_inputs(seed, part) draws one part's arguments, and reference() takes and returns one part's arrays. A program takes and returns all parts, laid end to end along the dimension named above; an argument that names none is the same for every part. Nothing has to cross between parts.
All inputs are finite; a program needn't handle non-finite values.
Results may differ from the reference program's by a relative error of at most 0.015.
The reference program's roundings to bfloat16 on the way count: a program that leaves them out, or rounds other values in their place, can miss the bound.
Values may be sent and summed in bfloat16 or wider, within the bound.
A program may use at most 128 MiB of HBM per device.

```python
import math
import jax
import jax.numpy as jnp
from jax import lax

D = 2048
HEAD = 64
SPAN = 64
SEQS = 2
TOK_DEV = 512
HEADS = 16
LENGTH = 2048
N_TP = 4


def draw_tokens(key, part):
    key_base, key_shift = jax.random.split(jax.random.fold_in(key, 11), 2)
    base = jax.random.normal(key_base, (LENGTH, SEQS, D), jnp.float32)
    shifts = 0.6 * jax.random.normal(key_shift, (LENGTH // TOK_DEV, SEQS, D), jnp.float32)
    base = base + jnp.repeat(shifts, TOK_DEV, axis=0)
    return jnp.clip(base, -64.0, 64.0).astype(jnp.bfloat16)


def steps_of(own_key, dims, cuts, smallest, high):
    loudness, own = 1.0, jax.random.fold_in(own_key, 6)
    for position, blocks in cuts:
        heights = jnp.exp(jax.random.uniform(jax.random.fold_in(own, position), (blocks,), jnp.float32, smallest / len(cuts), high / len(cuts)))
        loudness = loudness * jnp.repeat(heights, dims[position] // blocks).reshape([-1 if axis == position else 1 for axis in range(len(dims))])
    return loudness


def bell_draw(own_key, extent, spread, bound, shards=(), held_as=jnp.bfloat16):
    result = spread * jax.random.normal(own_key, extent, jnp.float32)
    if shards:
        result = result * steps_of(own_key, extent, shards, -0.22, 0.18)
    return jnp.clip(result, -bound, bound).astype(held_as)


def setup_inputs(seed: int = 0, part: int = 0) -> dict:
    keys = jax.random.split(jax.random.key(seed), 8)
    part_splits = jax.random.split(jax.random.fold_in(keys[7], part), 8)
    return {
        "tokens": draw_tokens(jax.random.fold_in(jax.random.fold_in(keys[7], part), 71), part),
        "w_query": bell_draw(keys[1], (D, D), (D // 3) ** -0.5, 0.21875, ((1, 4),)),
        "w_key": bell_draw(keys[2], (D, D), D ** -0.5, 0.125, ((1, 4),)),
        "w_value": bell_draw(keys[3], (D, D), D ** -0.5, 0.125, ((1, 4),)),
        "w_out": bell_draw(keys[4], (D, D), D ** -0.5, 0.125, ((0, 4),)),
        "head_lambda": jnp.clip(0.3 + 0.5 * jax.random.uniform(keys[5], (HEADS,), jnp.float32) ** steps_of(keys[5], (HEADS,), ((0, 4),), -0.2, 0.2), 0.3, 0.8),
        "sub_gain": jnp.clip(1.0 + 0.18 * jax.random.normal(keys[6], (2 * HEAD,), jnp.float32), 0.1, 1.9),
    }


def one_sequence(seq_tokens, w_query, w_key, w_value, w_out, head_lambda, sub_gain):
    total_rows = seq_tokens.shape[0]
    head_count = head_lambda.shape[0]
    value_dim = 2 * HEAD
    queries = jnp.dot(seq_tokens, w_query, preferred_element_type=jnp.float32).astype(jnp.bfloat16)
    queries = queries.reshape(total_rows, head_count, 2, HEAD).transpose(1, 0, 2, 3)
    keys_all = jnp.dot(seq_tokens, w_key, preferred_element_type=jnp.float32).astype(jnp.bfloat16)
    keys_all = keys_all.reshape(total_rows, head_count, 2, HEAD).transpose(1, 0, 2, 3)
    values = jnp.dot(seq_tokens, w_value, preferred_element_type=jnp.float32).astype(jnp.bfloat16)
    values = values.reshape(total_rows, head_count, value_dim).transpose(1, 0, 2)
    blk_len = math.gcd(total_rows, 512)
    blk_count = total_rows // blk_len
    positions = jnp.arange(total_rows, dtype=jnp.int32)

    def one_head(head_args):
        head_q, head_k, head_v, head_lam = head_args
        key_f = head_k.astype(jnp.float32)
        value_f = head_v.astype(jnp.float32)

        def one_block(blk_args):
            query_blk, blk_index = blk_args
            query_pos = blk_index * blk_len + jnp.arange(blk_len, dtype=jnp.int32)
            scores = jnp.einsum('qmd,kmd->mqk', query_blk.astype(jnp.float32), key_f) * HEAD ** (-0.5)
            allowed = (positions // SPAN)[None, :] <= (query_pos // SPAN)[:, None]
            top_val = lax.optimization_barrier(jnp.max(jnp.where(allowed, scores, -jnp.inf), axis=-1, keepdims=True))
            expo_vals = jnp.where(allowed, jnp.exp(scores - top_val), 0.0)
            sums = lax.optimization_barrier(jnp.sum(expo_vals, axis=-1))
            rounded = lax.optimization_barrier(expo_vals.astype(jnp.bfloat16)).astype(jnp.float32)
            accum = jnp.einsum('mqk,ke->mqe', rounded, value_f)
            return accum[0] / sums[0][:, None] - head_lam * accum[1] / sums[1][:, None]
        blocks_out = lax.map(one_block, (head_q.reshape(blk_count, blk_len, 2, HEAD), jnp.arange(blk_count, dtype=jnp.int32)))
        return blocks_out.reshape(total_rows, value_dim)
    attn = lax.map(one_head, (queries, keys_all, values, head_lambda))
    mean_sq = lax.optimization_barrier(jnp.mean(attn * attn, axis=-1, keepdims=True))
    normed = (attn * lax.rsqrt(mean_sq + 1e-06) * sub_gain).astype(jnp.bfloat16)
    normed = normed.transpose(1, 0, 2).reshape(total_rows, head_count * value_dim)
    group_cols = head_count * value_dim // N_TP
    summed = jnp.zeros((total_rows, w_out.shape[1]), jnp.float32)
    for group in range(N_TP):
        partial_out = jnp.dot(normed[:, group * group_cols:(group + 1) * group_cols], w_out[group * group_cols:(group + 1) * group_cols], preferred_element_type=jnp.float32)
        summed = summed + lax.optimization_barrier(partial_out.astype(jnp.bfloat16)).astype(jnp.float32)
    return summed.astype(jnp.bfloat16)

def reference(tokens, w_query, w_key, w_value, w_out, head_lambda, sub_gain):
    outputs = []
    for seq_index in range(tokens.shape[1]):
        outputs.append(one_sequence(tokens[:, seq_index], w_query, w_key, w_value, w_out, head_lambda, sub_gain))
    return jnp.stack(outputs, axis=1)
```

```python
import functools
import math

import jax
import jax.numpy as jnp
from jax import lax
from jax.experimental import pallas as pl
from jax.experimental.pallas import tpu as pltpu
from jax.sharding import PartitionSpec as P

SPAN = 64


NEG_FILL = -1e30
EPS_NORM = 1e-06


def key_block(state_in, queries, query_pos, key_blk, value_blk, key_start):
    run_max, run_sum, run_acc = state_in
    blk_len = key_blk.shape[0]
    heads_here = queries.shape[1]
    head_dim = queries.shape[3]
    key_pos = key_start + jnp.arange(blk_len, dtype=jnp.int32)
    key_four = key_blk.reshape(blk_len, heads_here, 2, head_dim)
    scores = jnp.einsum("qhmd,khmd->mhqk", queries, key_four, preferred_element_type=jnp.float32)
    scores = scores * head_dim ** (-0.5)
    allowed = (key_pos // SPAN)[None, :] <= (query_pos // SPAN)[:, None]
    new_max = jnp.maximum(run_max, jnp.max(jnp.where(allowed, scores, NEG_FILL), axis=-1))
    expo_vals = jnp.where(allowed, jnp.exp(scores - new_max[..., None]), 0.0)
    factor = jnp.exp(run_max - new_max)
    run_sum = run_sum * factor + jnp.sum(expo_vals, axis=-1)
    value_three = value_blk.reshape(blk_len, heads_here, 2 * head_dim)
    mixed_vals = jnp.einsum(
        "mhqk,khe->mhqe",
        expo_vals.astype(jnp.bfloat16),
        value_three,
        preferred_element_type=jnp.float32,
    )
    run_acc = run_acc * factor[..., None] + mixed_vals
    return (new_max, run_sum, run_acc)


def guarded_block(state_in, queries, query_pos, key_blk, value_blk, key_start):
    last_pos = query_pos[-1]

    def compute(inner_state):
        return key_block(inner_state, queries, query_pos, key_blk, value_blk, key_start)

    def keep(inner_state):
        return inner_state

    return lax.cond(key_start <= last_pos, compute, keep, state_in)


def sequence_piece(state_in, queries, query_pos, key_part, value_part):
    length = key_part.shape[0]
    step_len = math.gcd(length, 512)
    step_count = length // step_len

    def one_step(step_index, inner_state):
        offset = step_index * step_len
        key_blk = lax.dynamic_slice_in_dim(key_part, offset, step_len, 0)
        value_blk = lax.dynamic_slice_in_dim(value_part, offset, step_len, 0)
        return guarded_block(inner_state, queries, query_pos, key_blk, value_blk, offset)

    return lax.fori_loop(0, step_count, one_step, state_in)


def normalize(attn, sub_gain):
    mean_sq = jnp.mean(attn * attn, axis=-1, keepdims=True)
    normed = (attn * lax.rsqrt(mean_sq + EPS_NORM) * sub_gain).astype(jnp.bfloat16)
    return jnp.transpose(normed, (1, 0, 2)).reshape(attn.shape[1], attn.shape[0] * attn.shape[2])


def on_device(tokens, w_query, w_key, w_value, w_out, head_lambda, sub_gain):
    tp_count = lax.axis_size("tp")
    tok_rows = tokens.shape[0] * tp_count
    seq_count = tokens.shape[1]
    heads_here = head_lambda.shape[0]
    head_dim = w_query.shape[1] // (2 * heads_here)
    value_dim = 2 * head_dim
    query_cols = w_query.shape[1]
    w_joined = jnp.concatenate([w_query, w_key, w_value], axis=1)
    joined = jnp.dot(
        lax.all_gather(tokens, "tp", axis=0, tiled=True),
        w_joined,
        preferred_element_type=jnp.float32,
    ).astype(jnp.bfloat16)
    query_flat = joined[:, :, :query_cols]
    keys_here = joined[:, :, query_cols : 2 * query_cols]
    values_here = joined[:, :, 2 * query_cols :]
    sp_index = lax.axis_index("sp")
    own_first = sp_index * tok_rows
    lam_col = head_lambda[:, None, None]

    def attend(query_sets, first_rows):
        positions = [first + jnp.arange(tok_rows, dtype=jnp.int32) for first in first_rows]
        query_four = [qset.reshape(tok_rows, heads_here, 2, head_dim) for qset in query_sets]
        start_one = (
            jnp.full((2, heads_here, tok_rows), NEG_FILL, jnp.float32),
            jnp.zeros((2, heads_here, tok_rows), jnp.float32),
            jnp.zeros((2, heads_here, tok_rows, value_dim), jnp.float32),
        )
        start_state = tuple((start_one for seq_index in range(seq_count)))
        key_part = lax.all_gather(keys_here, "sp", axis=0, tiled=True)
        value_part = lax.all_gather(values_here, "sp", axis=0, tiled=True)
        new_states = []
        for seq_index in range(seq_count):
            new_states.append(
                sequence_piece(
                    start_state[seq_index],
                    query_four[seq_index],
                    positions[seq_index],
                    key_part[:, seq_index],
                    value_part[:, seq_index],
                )
            )
        final_states = tuple(new_states)
        results = []
        for run_max, run_sum, run_acc in final_states:
            attn = run_acc[0] / run_sum[0][..., None] - lam_col * run_acc[1] / run_sum[1][..., None]
            results.append(normalize(attn, sub_gain))
        return results

    normed_list = attend(
        [query_flat[:, seq_index] for seq_index in range(seq_count)],
        [own_first for seq_index in range(seq_count)],
    )
    normed = jnp.stack(normed_list, axis=1)
    return lax.psum_scatter(
        jnp.dot(normed, w_out, preferred_element_type=jnp.float32).astype(jnp.bfloat16),
        "tp",
        scatter_dimension=0,
        tiled=True,
    )


LANES = 128
LOG2E = 1.4426950408889634


def remote(src, dst, send, recv, where):
    return pltpu.make_async_remote_copy(
        src_ref=src,
        dst_ref=dst,
        send_sem=send,
        recv_sem=recv,
        device_id=where,
        device_id_type=pl.DeviceIdType.MESH,
    )


def layer_kernel(
    n_sp, n_tp, tok_ref, wq_ref, wk_ref, wv_ref, wo_ref, lam_ref, gain_ref, out_ref,
    tokbuf, wbuf, wfull, stage, recv, ostage, obuf,
    tok_send, tok_recv, tok_local, w_sem, wo_send, wo_recv, wo_local,
    x_send, x_recv, x_local, o_send, o_recv,
):
    z = lax.axis_index("sp")
    t = lax.axis_index("tp")
    n_x = n_tp // 2
    x = t // 2
    core = t % 2
    partner = x * 2 + (1 - core)
    seqs, rows, _ = tok_ref.shape
    heads = n_sp
    zrows = rows * n_tp
    prow = 2 * rows
    half = LANES // 2

    w_copies = [
        pltpu.make_async_copy(ref, wbuf.at[j], w_sem.at[j])
        for j, ref in enumerate((wq_ref, wk_ref, wv_ref))
    ]
    for cp in w_copies:
        cp.start()
    wo_copy = pltpu.make_async_copy(wo_ref, wfull.at[t], wo_local.at[0])
    wo_copy.start()
    own_copies = [
        pltpu.make_async_copy(tok_ref.at[s], tokbuf.at[s, t], tok_local.at[s]) for s in range(seqs)
    ]
    for cp in own_copies:
        cp.start()

    barrier = pltpu.get_barrier_semaphore()
    for dz in range(n_sp):
        for dt in range(n_tp):
            if dz or dt:
                pl.semaphore_signal(
                    barrier,
                    inc=1,
                    device_id={"sp": (z + dz) % n_sp, "tp": (t + dt) % n_tp},
                    device_id_type=pl.DeviceIdType.MESH,
                )
    pl.semaphore_wait(barrier, n_sp * n_tp - 1)

    def tok_x(s, k):
        return remote(
            tok_ref.at[s], tokbuf.at[s, t], tok_send.at[s, k], tok_recv.at[s, k],
            {"tp": ((x + k) % n_x) * 2 + core},
        )

    def tok_pair(s):
        return remote(
            tok_ref.at[s], tokbuf.at[s, t], tok_send.at[s, 0], tok_recv.at[s, 0], {"tp": partner}
        )

    def tok_forward(s, k):
        r = ((x + n_x - k) % n_x) * 2 + core
        return remote(
            tokbuf.at[s, r], tokbuf.at[s, r], tok_send.at[s, n_x - 1 + k],
            tok_recv.at[s, n_x - 1 + k], {"tp": partner},
        )

    def wo_x(k):
        return remote(
            wo_ref, wfull.at[t], wo_send.at[k], wo_recv.at[k], {"tp": ((x + k) % n_x) * 2 + core}
        )

    def wo_pair():
        return remote(wo_ref, wfull.at[t], wo_send.at[0], wo_recv.at[0], {"tp": partner})

    def wo_forward(k):
        r = ((x + n_x - k) % n_x) * 2 + core
        return remote(
            wfull.at[r], wfull.at[r], wo_send.at[n_x - 1 + k], wo_recv.at[n_x - 1 + k],
            {"tp": partner},
        )

    for s in range(seqs):
        for k in range(1, n_x):
            tok_x(s, k).start()
        tok_pair(s).start()
    for k in range(1, n_x):
        wo_x(k).start()

    def row_of(z_src, k):
        xk = (x + n_x - k) % n_x
        return pl.multiple_of(z_src * zrows + xk * prow, prow)

    def x_copy(s, k, d):
        zd = (z + d) % n_sp
        return remote(
            stage.at[s, k, zd], recv.at[s, :, pl.ds(row_of(z, k), prow), :],
            x_send.at[s, k, d - 1], x_recv.at[s, k, d - 1], {"sp": zd},
        )

    def x_own(s, k):
        return pltpu.make_async_copy(
            stage.at[s, k, z], recv.at[s, :, pl.ds(row_of(z, k), prow), :], x_local.at[s, k]
        )

    def project(s, k):
        xk = (x + n_x - k) % n_x
        lhs = tokbuf.at[s, pl.ds(xk * 2, 2)]

        def one(j, _):
            got = jnp.dot(
                lhs[...].reshape(prow, tokbuf.shape[3]), wbuf[j],
                preferred_element_type=jnp.float32,
            ).astype(jnp.bfloat16)
            for h in range(heads):
                stage[s, k, h, j] = got[:, h * LANES : (h + 1) * LANES]
            return 0

        lax.fori_loop(0, 3, one, 0)
        for d in range(1, n_sp):
            x_copy(s, k, d).start()
        x_own(s, k).start()

    for s in range(seqs):
        own_copies[s].wait()
        tok_pair(s).wait_recv()
        if s == 0:
            for cp in w_copies:
                cp.wait()
        project(s, 0)
        for k in range(1, n_x):
            tok_x(s, k).wait_recv()
            tok_forward(s, k).start()
        for k in range(1, n_x):
            tok_forward(s, k).wait_recv()
            project(s, k)
    wo_pair().start()

    lam = lam_ref[z]
    gain = gain_ref[...]
    scale = half ** (-0.5) * LOG2E
    head_id = t * heads + z
    head_cols = pl.ds(pl.multiple_of(head_id * LANES, LANES), LANES)
    lane = lax.broadcasted_iota(jnp.int32, (zrows, LANES), 1)
    first_map = lane < half

    def o_copy(s, qi, dt):
        td = (t + dt) % n_tp
        src = ostage.at[s, qi, td]
        return remote(
            src, obuf.at[s, :, head_cols], o_send.at[s, qi, dt], o_recv.at[s, head_id],
            {"sp": qi, "tp": td},
        )

    def o_own(s):
        return pltpu.make_async_copy(
            ostage.at[s, z, t], obuf.at[s, :, head_cols], o_recv.at[s, head_id]
        )

    def attend(s):
        def key_step(start, qs, state, masked):
            sl = pl.ds(start, zrows)
            sc = lax.dot_general(
                qs, recv[s, 1, sl, :], (((1,), (1,)), ((), ())),
                preferred_element_type=jnp.float32,
            )
            if masked:
                row = lax.broadcasted_iota(jnp.int32, sc.shape, 0) % zrows
                col = lax.broadcasted_iota(jnp.int32, sc.shape, 1)
                sc = jnp.where(col // SPAN <= row // SPAN, sc, NEG_FILL)
            top = jnp.max(sc, axis=-1, keepdims=True)
            if state is not None:
                top = jnp.maximum(top, state[0])
            ex = jnp.exp2((sc - top) * scale)
            tot = jnp.sum(ex, axis=-1, keepdims=True)
            acc = jnp.dot(
                ex.astype(jnp.bfloat16), recv[s, 2, sl, :], preferred_element_type=jnp.float32
            )
            if state is not None:
                factor = jnp.exp2((state[0] - top) * scale)
                tot = tot + state[1] * factor
                acc = acc + state[2] * factor
            return top, tot, acc

        def q_step(qi, _):
            start = pl.multiple_of(qi * zrows, zrows)
            q = recv[s, 0, pl.ds(start, zrows), :]
            zero = jnp.zeros_like(q)
            qs = jnp.concatenate(
                [jnp.where(first_map, q, zero), jnp.where(first_map, zero, q)], axis=0
            )
            state = key_step(start, qs, None, True)

            def full(kj, inner):
                return key_step(pl.multiple_of(kj * zrows, zrows), qs, inner, False)

            _, tot, acc = lax.fori_loop(0, qi, full, state)
            attn = acc[:zrows] / tot[:zrows] - lam * acc[zrows:] / tot[zrows:]
            mean_sq = jnp.mean(attn * attn, axis=-1, keepdims=True)
            normed = (attn * lax.rsqrt(mean_sq + EPS_NORM) * gain).astype(jnp.bfloat16)
            ostage[s, qi] = normed.reshape(n_tp, rows, LANES)
            for dt in range(1, n_tp):
                o_copy(s, qi, dt).start()

            @pl.when(qi == z)
            def _():
                o_own(s).start()

            @pl.when(qi != z)
            def _():
                o_copy(s, qi, 0).start()

            return 0

        lax.fori_loop(0, n_sp, q_step, 0)

    def wait_x(s):
        for k in range(n_x):
            x_own(s, k).wait()
            for d in range(1, n_sp):
                zs = (z + n_sp - d) % n_sp
                remote(
                    stage.at[s, k, 0], recv.at[s, :, pl.ds(row_of(zs, k), prow), :],
                    x_send.at[s, k, d - 1], x_recv.at[s, k, d - 1], {"sp": zs},
                ).wait_recv()

    def finish(s):
        def one(g, _):
            cols = pl.ds(pl.multiple_of(g * LANES, LANES), LANES)
            pltpu.make_async_copy(
                ostage.at[s, 0, 0], obuf.at[s, :, cols], o_recv.at[s, g]
            ).wait()
            return 0

        lax.fori_loop(0, n_tp * heads, one, 0)
        width = heads * LANES
        total = jnp.zeros((rows, out_ref.shape[2]), jnp.float32)
        for g in range(n_tp):
            part = jnp.dot(
                obuf[s, :, g * width : (g + 1) * width], wfull[g],
                preferred_element_type=jnp.float32,
            )
            total = total + part.astype(jnp.bfloat16).astype(jnp.float32)
        out_ref[s] = total.astype(out_ref.dtype)

    for s in range(seqs):
        wait_x(s)
        if s == seqs - 1:
            for k in range(1, n_x):
                wo_x(k).wait_recv()
                wo_forward(k).start()
        attend(s)
    wo_copy.wait()
    wo_pair().wait_recv()
    for k in range(1, n_x):
        wo_forward(k).wait_recv()
    for s in range(seqs):
        finish(s)

    for s in range(seqs):
        tok_pair(s).wait_send()
        for k in range(1, n_x):
            tok_x(s, k).wait_send()
            tok_forward(s, k).wait_send()
        for k in range(n_x):
            for d in range(1, n_sp):
                x_copy(s, k, d).wait_send()

        def sent(qi, _, s=s):
            for dt in range(1, n_tp):
                o_copy(s, qi, dt).wait_send()

            @pl.when(qi != z)
            def _():
                o_copy(s, qi, 0).wait_send()

            return 0

        lax.fori_loop(0, n_sp, sent, 0)
    wo_pair().wait_send()
    for k in range(1, n_x):
        wo_x(k).wait_send()
        wo_forward(k).wait_send()


def fused_device(n_sp, n_tp, tokens, w_query, w_key, w_value, w_out, head_lambda, sub_gain):
    rows, seqs, width = tokens.shape
    cols = w_query.shape[1]
    n_x = n_tp // 2
    heads = head_lambda.shape[0]
    bf = jnp.bfloat16
    dma = pltpu.SemaphoreType.DMA
    any_spec = pl.BlockSpec(memory_space=pl.ANY)
    vmem_spec = pl.BlockSpec(memory_space=pltpu.VMEM)
    out = pl.pallas_call(
        functools.partial(layer_kernel, n_sp, n_tp),
        out_shape=jax.ShapeDtypeStruct((seqs, rows, w_out.shape[1]), bf),
        in_specs=[
            vmem_spec, any_spec, any_spec, any_spec, any_spec,
            pl.BlockSpec(memory_space=pltpu.SMEM), vmem_spec,
        ],
        out_specs=vmem_spec,
        scratch_shapes=[
            pltpu.VMEM((seqs, n_tp, rows, width), bf),
            pltpu.VMEM((3, width, cols), bf),
            pltpu.VMEM((n_tp,) + w_out.shape, bf),
            pltpu.VMEM((seqs, n_x, heads, 3, 2 * rows, LANES), bf),
            pltpu.VMEM((seqs, 3, rows * n_tp * n_sp, LANES), bf),
            pltpu.VMEM((seqs, n_sp, n_tp, rows, LANES), bf),
            pltpu.VMEM((seqs, rows, n_tp * heads * LANES), bf),
            dma((seqs, 2 * n_x)),
            dma((seqs, 2 * n_x)),
            dma((seqs,)),
            dma((3,)),
            dma((2 * n_x,)),
            dma((2 * n_x,)),
            dma((1,)),
            dma((seqs, n_x, n_sp)),
            dma((seqs, n_x, n_sp)),
            dma((seqs, n_x)),
            dma((seqs, n_sp, n_tp)),
            dma((seqs, n_tp * heads)),
        ],
        compiler_params=pltpu.CompilerParams(
            collective_id=0, has_side_effects=True, vmem_limit_bytes=58 * 2**20
        ),
    )(
        jnp.transpose(tokens, (1, 0, 2)), w_query, w_key, w_value, w_out,
        head_lambda, sub_gain.reshape(1, -1),
    )
    return jnp.transpose(out, (1, 0, 2))


def layer(tokens, w_query, w_key, w_value, w_out, head_lambda, sub_gain):
    args = (tokens, w_query, w_key, w_value, w_out, head_lambda, sub_gain)
    n_sp, n_tp = lax.axis_size("sp"), lax.axis_size("tp")
    heads = head_lambda.shape[0]
    fits = (
        heads == n_sp
        and n_sp > 1
        and n_tp % 2 == 0
        and w_query.shape[1] == heads * LANES
        and sub_gain.shape[0] == LANES
        and tokens.shape[0] % 16 == 0
        and (tokens.shape[0] * n_tp) % SPAN == 0
    )
    if fits:
        return fused_device(n_sp, n_tp, *args)
    return on_device(*args)


def solution(mesh):
    return jax.shard_map(
        layer,
        mesh=mesh,
        in_specs=(
            P(("grp", "sp", "tp"), None, None),
            P(None, "tp"),
            P(None, "tp"),
            P(None, "tp"),
            P("tp", None),
            P("tp"),
            P(),
        ),
        out_specs=P(("grp", "sp", "tp"), None, None),
        check_vma=False,
    )
```

```python
import functools
import math

import jax
import jax.numpy as jnp
from jax import lax
from jax.experimental import pallas as pl
from jax.experimental.pallas import tpu as pltpu
from jax.sharding import PartitionSpec as P

SPAN = 64


NEG_FILL = -1e30
EPS_NORM = 1e-06


def key_block(state_in, queries, query_pos, key_blk, value_blk, key_start):
    run_max, run_sum, run_acc = state_in
    blk_len = key_blk.shape[0]
    heads_here = queries.shape[1]
    head_dim = queries.shape[3]
    key_pos = key_start + jnp.arange(blk_len, dtype=jnp.int32)
    key_four = key_blk.reshape(blk_len, heads_here, 2, head_dim)
    scores = jnp.einsum("qhmd,khmd->mhqk", queries, key_four, preferred_element_type=jnp.float32)
    scores = scores * head_dim ** (-0.5)
    allowed = (key_pos // SPAN)[None, :] <= (query_pos // SPAN)[:, None]
    new_max = jnp.maximum(run_max, jnp.max(jnp.where(allowed, scores, NEG_FILL), axis=-1))
    expo_vals = jnp.where(allowed, jnp.exp(scores - new_max[..., None]), 0.0)
    factor = jnp.exp(run_max - new_max)
    run_sum = run_sum * factor + jnp.sum(expo_vals, axis=-1)
    value_three = value_blk.reshape(blk_len, heads_here, 2 * head_dim)
    mixed_vals = jnp.einsum(
        "mhqk,khe->mhqe",
        expo_vals.astype(jnp.bfloat16),
        value_three,
        preferred_element_type=jnp.float32,
    )
    run_acc = run_acc * factor[..., None] + mixed_vals
    return (new_max, run_sum, run_acc)


def guarded_block(state_in, queries, query_pos, key_blk, value_blk, key_start):
    last_pos = query_pos[-1]

    def compute(inner_state):
        return key_block(inner_state, queries, query_pos, key_blk, value_blk, key_start)

    def keep(inner_state):
        return inner_state

    return lax.cond(key_start <= last_pos, compute, keep, state_in)


def sequence_piece(state_in, queries, query_pos, key_part, value_part):
    length = key_part.shape[0]
    step_len = math.gcd(length, 512)
    step_count = length // step_len

    def one_step(step_index, inner_state):
        offset = step_index * step_len
        key_blk = lax.dynamic_slice_in_dim(key_part, offset, step_len, 0)
        value_blk = lax.dynamic_slice_in_dim(value_part, offset, step_len, 0)
        return guarded_block(inner_state, queries, query_pos, key_blk, value_blk, offset)

    return lax.fori_loop(0, step_count, one_step, state_in)


def normalize(attn, sub_gain):
    mean_sq = jnp.mean(attn * attn, axis=-1, keepdims=True)
    normed = (attn * lax.rsqrt(mean_sq + EPS_NORM) * sub_gain).astype(jnp.bfloat16)
    return jnp.transpose(normed, (1, 0, 2)).reshape(attn.shape[1], attn.shape[0] * attn.shape[2])


def on_device(tokens, w_query, w_key, w_value, w_out, head_lambda, sub_gain):
    tp_count = lax.axis_size("tp")
    tok_rows = tokens.shape[0] * tp_count
    seq_count = tokens.shape[1]
    heads_here = head_lambda.shape[0]
    head_dim = w_query.shape[1] // (2 * heads_here)
    value_dim = 2 * head_dim
    query_cols = w_query.shape[1]
    w_joined = jnp.concatenate([w_query, w_key, w_value], axis=1)
    joined = jnp.dot(
        lax.all_gather(tokens, "tp", axis=0, tiled=True),
        w_joined,
        preferred_element_type=jnp.float32,
    ).astype(jnp.bfloat16)
    query_flat = joined[:, :, :query_cols]
    keys_here = joined[:, :, query_cols : 2 * query_cols]
    values_here = joined[:, :, 2 * query_cols :]
    sp_index = lax.axis_index("sp")
    own_first = sp_index * tok_rows
    lam_col = head_lambda[:, None, None]

    def attend(query_sets, first_rows):
        positions = [first + jnp.arange(tok_rows, dtype=jnp.int32) for first in first_rows]
        query_four = [qset.reshape(tok_rows, heads_here, 2, head_dim) for qset in query_sets]
        start_one = (
            jnp.full((2, heads_here, tok_rows), NEG_FILL, jnp.float32),
            jnp.zeros((2, heads_here, tok_rows), jnp.float32),
            jnp.zeros((2, heads_here, tok_rows, value_dim), jnp.float32),
        )
        start_state = tuple((start_one for seq_index in range(seq_count)))
        key_part = lax.all_gather(keys_here, "sp", axis=0, tiled=True)
        value_part = lax.all_gather(values_here, "sp", axis=0, tiled=True)
        new_states = []
        for seq_index in range(seq_count):
            new_states.append(
                sequence_piece(
                    start_state[seq_index],
                    query_four[seq_index],
                    positions[seq_index],
                    key_part[:, seq_index],
                    value_part[:, seq_index],
                )
            )
        final_states = tuple(new_states)
        results = []
        for run_max, run_sum, run_acc in final_states:
            attn = run_acc[0] / run_sum[0][..., None] - lam_col * run_acc[1] / run_sum[1][..., None]
            results.append(normalize(attn, sub_gain))
        return results

    normed_list = attend(
        [query_flat[:, seq_index] for seq_index in range(seq_count)],
        [own_first for seq_index in range(seq_count)],
    )
    normed = jnp.stack(normed_list, axis=1)
    return lax.psum_scatter(
        jnp.dot(normed, w_out, preferred_element_type=jnp.float32).astype(jnp.bfloat16),
        "tp",
        scatter_dimension=0,
        tiled=True,
    )


LANES = 128
LOG2E = 1.4426950408889634


def remote(src, dst, send, recv, where):
    return pltpu.make_async_remote_copy(
        src_ref=src,
        dst_ref=dst,
        send_sem=send,
        recv_sem=recv,
        device_id=where,
        device_id_type=pl.DeviceIdType.MESH,
    )


def layer_kernel(
    n_grp, n_sp, n_tp, tok_ref, wq_ref, wk_ref, wv_ref, wo_ref, lam_ref, gain_ref, out_ref,
    tokbuf, wbuf, wfull, stage, recv, kvx, ostage, olocal, obuf,
    tok_send, tok_recv, tok_local, w_sem, wo_send, wo_recv, wo_local,
    x_send, x_recv, q_send, q_recv, x_local, e_send, e_recv, o_send, ol_send, o_recv,
):
    grp = lax.axis_index("grp")
    z = lax.axis_index("sp")
    low = n_sp // 2
    t = lax.axis_index("tp")
    n_x = n_tp // 2
    x = t // 2
    core = t % 2
    partner = x * 2 + (1 - core)
    seqs, rows, _ = tok_ref.shape
    heads = n_sp
    zrows = rows * n_tp
    prow = 2 * rows
    half = LANES // 2

    w_copies = [
        pltpu.make_async_copy(ref, wbuf.at[j], w_sem.at[j])
        for j, ref in enumerate((wq_ref, wk_ref, wv_ref))
    ]
    for cp in w_copies:
        cp.start()
    wo_copy = pltpu.make_async_copy(wo_ref, wfull.at[t], wo_local.at[0])
    wo_copy.start()
    own_copies = [
        pltpu.make_async_copy(tok_ref.at[s], tokbuf.at[s, t], tok_local.at[s]) for s in range(seqs)
    ]
    for cp in own_copies:
        cp.start()

    barrier = pltpu.get_barrier_semaphore()
    for dz in range(n_sp):
        for dt in range(n_tp):
            if dz or dt:
                pl.semaphore_signal(
                    barrier,
                    inc=1,
                    device_id={"sp": (z + dz) % n_sp, "tp": (t + dt) % n_tp},
                    device_id_type=pl.DeviceIdType.MESH,
                )
    for e in range(1, n_grp):
        pl.semaphore_signal(
            barrier, inc=1, device_id={"grp": (grp + e) % n_grp},
            device_id_type=pl.DeviceIdType.MESH,
        )
    pl.semaphore_wait(barrier, n_sp * n_tp + n_grp - 2)

    def tok_x(s, k):
        return remote(
            tok_ref.at[s], tokbuf.at[s, t], tok_send.at[s, k], tok_recv.at[s, k],
            {"tp": ((x + k) % n_x) * 2 + core},
        )

    def tok_pair(s):
        return remote(
            tok_ref.at[s], tokbuf.at[s, t], tok_send.at[s, 0], tok_recv.at[s, 0], {"tp": partner}
        )

    def tok_forward(s, k):
        r = ((x + n_x - k) % n_x) * 2 + core
        return remote(
            tokbuf.at[s, r], tokbuf.at[s, r], tok_send.at[s, n_x - 1 + k],
            tok_recv.at[s, n_x - 1 + k], {"tp": partner},
        )

    part_rows = wo_ref.shape[0] // n_grp

    def part(e):
        return pl.ds(pl.multiple_of(((grp + n_grp - e) % n_grp) * part_rows, part_rows), part_rows)

    def wo_x(k):
        return remote(
            wo_ref.at[part(0)], wfull.at[t, part(0)], wo_send.at[k, 0, 0], wo_recv.at[k, 0, 0],
            {"tp": ((x + k) % n_x) * 2 + core},
        )

    def wo_pair():
        return remote(
            wo_ref, wfull.at[t], wo_send.at[0, 0, 0], wo_recv.at[0, 0, 0], {"tp": partner}
        )

    def wo_grp(k, e):
        blk = wfull.at[((x + n_x - k) % n_x) * 2 + core, part(0)]
        return remote(
            blk, blk, wo_send.at[k, 0, e], wo_recv.at[k, 0, e], {"grp": (grp + e) % n_grp}
        )

    def wo_forward(k, e):
        blk = wfull.at[((x + n_x - k) % n_x) * 2 + core, part(e)]
        return remote(blk, blk, wo_send.at[k, 1, e], wo_recv.at[k, 1, e], {"tp": partner})

    for s in range(seqs):
        for k in range(1, n_x):
            tok_x(s, k).start()
        tok_pair(s).start()
    for k in range(1, n_x):
        wo_x(k).start()

    def x_of(k):
        return (x + n_x - k) % n_x

    def row_of(z_src, k):
        return pl.multiple_of(z_src * zrows + x_of(k) * prow, prow)

    def stays(row_shard, home):
        return (home != row_shard) & (
            (row_shard == 0) | ((row_shard < low) & (home >= low))
        )

    def kv_copy(s, k, d):
        zd = (z + d) % n_sp
        return remote(
            stage.at[s, x_of(k), zd, pl.ds(1, 2)],
            recv.at[s, pl.ds(1, 2), pl.ds(row_of(z, k), prow), :],
            x_send.at[s, k, d - 1], x_recv.at[s, k, d - 1], {"sp": zd},
        )

    def q_copy(s, k, d):
        zd = (z + d) % n_sp
        return remote(
            stage.at[s, x_of(k), zd, 0], recv.at[s, 0, pl.ds(row_of(z, k), prow), :],
            q_send.at[s, k, d - 1], q_recv.at[s, k, d - 1], {"sp": zd},
        )

    def extra_copy(s, k, i):
        return remote(
            stage.at[s, x_of(k), low + i, pl.ds(1, 2)], kvx.at[s, i, :, x_of(k)],
            e_send.at[s, k, i], e_recv.at[s, k, i], {"sp": 1},
        )

    def x_own(s, k):
        return pltpu.make_async_copy(
            stage.at[s, x_of(k), z], recv.at[s, :, pl.ds(row_of(z, k), prow), :],
            x_local.at[s, k],
        )

    def project(s, k):
        lhs = tokbuf.at[s, pl.ds(x_of(k) * 2, 2)]

        def one(j, _):
            got = jnp.dot(
                lhs[...].reshape(prow, tokbuf.shape[3]), wbuf[j],
                preferred_element_type=jnp.float32,
            ).astype(jnp.bfloat16)
            for h in range(heads):
                stage[s, x_of(k), h, j] = got[:, h * LANES : (h + 1) * LANES]
            return 0

        lax.fori_loop(0, 3, one, 0)
        for d in range(1, n_sp):
            kv_copy(s, k, d).start()

            @pl.when(jnp.logical_not(stays(z, (z + d) % n_sp)))
            def _(d=d):
                q_copy(s, k, d).start()

        @pl.when(z == 0)
        def _():
            for i in range(heads - low):
                extra_copy(s, k, i).start()

        x_own(s, k).start()

    for s in range(seqs):
        own_copies[s].wait()
        tok_pair(s).wait_recv()
        if s == 0:
            for cp in w_copies:
                cp.wait()
        project(s, 0)
        for k in range(1, n_x):
            tok_x(s, k).wait_recv()
            tok_forward(s, k).start()
        for k in range(1, n_x):
            tok_forward(s, k).wait_recv()
            project(s, k)
    wo_pair().start()

    gain = gain_ref[...]
    scale = half ** (-0.5) * LOG2E
    head_id = t * heads + z
    head_cols = pl.ds(pl.multiple_of(head_id * LANES, LANES), LANES)
    lane = lax.broadcasted_iota(jnp.int32, (zrows, LANES), 1)
    first_map = lane < half

    def o_copy(s, qi, dt):
        td = (t + dt) % n_tp
        src = ostage.at[s, qi, td]
        return remote(
            src, obuf.at[s, :, head_cols], o_send.at[s, qi, dt], o_recv.at[s, head_id],
            {"sp": qi, "tp": td},
        )

    def o_own(s):
        return pltpu.make_async_copy(
            ostage.at[s, z, t], obuf.at[s, :, head_cols], o_recv.at[s, head_id]
        )

    def key_step(qs, keys, vals, state, masked):
        sc = lax.dot_general(
            qs, keys, (((1,), (1,)), ((), ())), preferred_element_type=jnp.float32
        )
        if masked:
            row = lax.broadcasted_iota(jnp.int32, sc.shape, 0) % zrows
            col = lax.broadcasted_iota(jnp.int32, sc.shape, 1)
            sc = jnp.where(col // SPAN <= row // SPAN, sc, NEG_FILL)
        top = jnp.max(sc, axis=-1, keepdims=True)
        if state is not None:
            top = jnp.maximum(top, state[0])
        ex = jnp.exp2((sc - top) * scale)
        tot = jnp.sum(ex, axis=-1, keepdims=True)
        acc = jnp.dot(ex.astype(jnp.bfloat16), vals, preferred_element_type=jnp.float32)
        if state is not None:
            factor = jnp.exp2((state[0] - top) * scale)
            tot = tot + state[1] * factor
            acc = acc + state[2] * factor
        return top, tot, acc

    def both_maps(q):
        zero = jnp.zeros_like(q)
        return jnp.concatenate(
            [jnp.where(first_map, q, zero), jnp.where(first_map, zero, q)], axis=0
        )

    def close(state, lam):
        _, tot, acc = state
        attn = acc[:zrows] / tot[:zrows] - lam * acc[zrows:] / tot[zrows:]
        mean_sq = jnp.mean(attn * attn, axis=-1, keepdims=True)
        normed = (attn * lax.rsqrt(mean_sq + EPS_NORM) * gain).astype(jnp.bfloat16)
        return normed.reshape(n_tp, rows, LANES)

    def attend(s):
        def q_step(step, _):
            qi = n_sp - 1 - step
            start = pl.multiple_of(qi * zrows, zrows)

            def block(j, first):
                return recv[s, j, pl.ds(pl.multiple_of(first, zrows), zrows), :]

            qs = both_maps(block(0, start))
            state = key_step(qs, block(1, start), block(2, start), None, True)

            def full(kj, inner):
                return key_step(qs, block(1, kj * zrows), block(2, kj * zrows), inner, False)

            ostage[s, qi] = close(lax.fori_loop(0, qi, full, state), lam_ref[z])
            for dt in range(1, n_tp):
                o_copy(s, qi, dt).start()

            @pl.when(qi == z)
            def _():
                o_own(s).start()

            @pl.when(qi != z)
            def _():
                o_copy(s, qi, 0).start()

            return 0

        lax.fori_loop(0, n_sp - jnp.minimum(z, low), q_step, 0)

    first_local = jnp.where(z < low, z + 1, heads)

    def local_cols(h):
        return pl.ds(pl.multiple_of((t * heads + h) * LANES, LANES), LANES)

    def ol_copy(s, h, dt):
        td = (t + dt) % n_tp
        return remote(
            olocal.at[s, h, td], obuf.at[s, :, local_cols(h)], ol_send.at[s, h, dt],
            o_recv.at[s, t * heads + h], {"tp": td},
        )

    def ol_own(s, h):
        return pltpu.make_async_copy(
            olocal.at[s, h, t], obuf.at[s, :, local_cols(h)], o_recv.at[s, t * heads + h]
        )

    def attend_local(s):
        @pl.when(z == 1)
        def _():
            for k in range(n_x):
                for i in range(heads - low):
                    extra_copy(s, k, i).wait_recv()

        def h_step(h, _):
            def own(j):
                return stage[s, :, h, j].reshape(zrows, LANES)

            qs = both_maps(own(0))
            state = key_step(qs, own(1), own(2), None, True)

            def before(i, inner):
                keys = kvx[s, h - low, 0].reshape(zrows, LANES)
                vals = kvx[s, h - low, 1].reshape(zrows, LANES)
                return key_step(qs, keys, vals, inner, False)

            olocal[s, h] = close(lax.fori_loop(0, z, before, state), lam_ref[h])
            for dt in range(1, n_tp):
                ol_copy(s, h, dt).start()
            ol_own(s, h).start()
            return 0

        lax.fori_loop(first_local, heads, h_step, 0)

    def wait_x(s):
        for k in range(n_x):
            x_own(s, k).wait()
            for d in range(1, n_sp):
                zs = (z + n_sp - d) % n_sp
                at = pl.ds(row_of(zs, k), prow)
                remote(
                    stage.at[s, 0, 0, pl.ds(1, 2)], recv.at[s, pl.ds(1, 2), at, :],
                    x_send.at[s, k, d - 1], x_recv.at[s, k, d - 1], {"sp": zs},
                ).wait_recv()

                @pl.when(jnp.logical_not(stays(zs, z)))
                def _(k=k, d=d, zs=zs, at=at):
                    remote(
                        stage.at[s, 0, 0, 0], recv.at[s, 0, at, :],
                        q_send.at[s, k, d - 1], q_recv.at[s, k, d - 1], {"sp": zs},
                    ).wait_recv()

    def finish(s):
        def one(g, _):
            cols = pl.ds(pl.multiple_of(g * LANES, LANES), LANES)
            pltpu.make_async_copy(
                ostage.at[s, 0, 0], obuf.at[s, :, cols], o_recv.at[s, g]
            ).wait()
            return 0

        lax.fori_loop(0, n_tp * heads, one, 0)
        width = heads * LANES
        total = jnp.zeros((rows, out_ref.shape[2]), jnp.float32)
        for g in range(n_tp):
            part = jnp.dot(
                obuf[s, :, g * width : (g + 1) * width], wfull[g],
                preferred_element_type=jnp.float32,
            )
            total = total + part.astype(jnp.bfloat16).astype(jnp.float32)
        out_ref[s] = total.astype(out_ref.dtype)

    for s in range(seqs):
        if s < seqs - 1:
            attend_local(s)
        else:

            @pl.when(z == 0)
            def _(s=s):
                attend_local(s)

        wait_x(s)
        if s == seqs - 1:
            for k in range(1, n_x):
                for e in range(1, n_grp):
                    wo_grp(k, e).wait_recv()
                    wo_forward(k, e).start()
        attend(s)
        if s == 0:
            for k in range(1, n_x):
                wo_x(k).wait_recv()
                for e in range(1, n_grp):
                    wo_grp(k, e).start()
                wo_forward(k, 0).start()

    @pl.when(z != 0)
    def _():
        attend_local(seqs - 1)

    wo_copy.wait()
    wo_pair().wait_recv()
    for k in range(1, n_x):
        for e in range(n_grp):
            wo_forward(k, e).wait_recv()
    for s in range(seqs):
        finish(s)

    for s in range(seqs):
        tok_pair(s).wait_send()
        for k in range(1, n_x):
            tok_x(s, k).wait_send()
            tok_forward(s, k).wait_send()
        for k in range(n_x):
            for d in range(1, n_sp):
                kv_copy(s, k, d).wait_send()

                @pl.when(jnp.logical_not(stays(z, (z + d) % n_sp)))
                def _(s=s, k=k, d=d):
                    q_copy(s, k, d).wait_send()

            @pl.when(z == 0)
            def _(s=s, k=k):
                for i in range(heads - low):
                    extra_copy(s, k, i).wait_send()

        def sent(step, _, s=s):
            qi = n_sp - 1 - step
            for dt in range(1, n_tp):
                o_copy(s, qi, dt).wait_send()

            @pl.when(qi != z)
            def _():
                o_copy(s, qi, 0).wait_send()

            return 0

        lax.fori_loop(0, n_sp - jnp.minimum(z, low), sent, 0)

        def local_sent(h, _, s=s):
            for dt in range(1, n_tp):
                ol_copy(s, h, dt).wait_send()
            return 0

        lax.fori_loop(first_local, heads, local_sent, 0)
    wo_pair().wait_send()
    for k in range(1, n_x):
        wo_x(k).wait_send()
        for e in range(n_grp):
            wo_forward(k, e).wait_send()
            if e:
                wo_grp(k, e).wait_send()


def fused_device(n_grp, n_sp, n_tp, tokens, w_query, w_key, w_value, w_out, head_lambda, sub_gain):
    rows, seqs, width = tokens.shape
    cols = w_query.shape[1]
    n_x = n_tp // 2
    heads = head_lambda.shape[0]
    bf = jnp.bfloat16
    dma = pltpu.SemaphoreType.DMA
    any_spec = pl.BlockSpec(memory_space=pl.ANY)
    vmem_spec = pl.BlockSpec(memory_space=pltpu.VMEM)
    out = pl.pallas_call(
        functools.partial(layer_kernel, n_grp, n_sp, n_tp),
        out_shape=jax.ShapeDtypeStruct((seqs, rows, w_out.shape[1]), bf),
        in_specs=[
            vmem_spec, any_spec, any_spec, any_spec, any_spec,
            pl.BlockSpec(memory_space=pltpu.SMEM), vmem_spec,
        ],
        out_specs=vmem_spec,
        scratch_shapes=[
            pltpu.VMEM((seqs, n_tp, rows, width), bf),
            pltpu.VMEM((3, width, cols), bf),
            pltpu.VMEM((n_tp,) + w_out.shape, bf),
            pltpu.VMEM((seqs, n_x, heads, 3, 2 * rows, LANES), bf),
            pltpu.VMEM((seqs, 3, rows * n_tp * n_sp, LANES), bf),
            pltpu.VMEM((seqs, heads - n_sp // 2, 2, n_x, 2 * rows, LANES), bf),
            pltpu.VMEM((seqs, n_sp, n_tp, rows, LANES), bf),
            pltpu.VMEM((seqs, heads, n_tp, rows, LANES), bf),
            pltpu.VMEM((seqs, rows, n_tp * heads * LANES), bf),
            dma((seqs, 2 * n_x)),
            dma((seqs, 2 * n_x)),
            dma((seqs,)),
            dma((3,)),
            dma((n_x, 2, n_grp)),
            dma((n_x, 2, n_grp)),
            dma((1,)),
            dma((seqs, n_x, n_sp)),
            dma((seqs, n_x, n_sp)),
            dma((seqs, n_x, n_sp)),
            dma((seqs, n_x, n_sp)),
            dma((seqs, n_x)),
            dma((seqs, n_x, heads)),
            dma((seqs, n_x, heads)),
            dma((seqs, n_sp, n_tp)),
            dma((seqs, heads, n_tp)),
            dma((seqs, n_tp * heads)),
        ],
        compiler_params=pltpu.CompilerParams(
            collective_id=0, has_side_effects=True, vmem_limit_bytes=58 * 2**20
        ),
    )(
        jnp.transpose(tokens, (1, 0, 2)), w_query, w_key, w_value, w_out,
        head_lambda, sub_gain.reshape(1, -1),
    )
    return jnp.transpose(out, (1, 0, 2))


def layer(tokens, w_query, w_key, w_value, w_out, head_lambda, sub_gain):
    args = (tokens, w_query, w_key, w_value, w_out, head_lambda, sub_gain)
    n_sp, n_tp = lax.axis_size("sp"), lax.axis_size("tp")
    heads = head_lambda.shape[0]
    fits = (
        heads == n_sp
        and n_sp == 4
        and w_out.shape[0] % 16 == 0
        and n_tp % 2 == 0
        and w_query.shape[1] == heads * LANES
        and sub_gain.shape[0] == LANES
        and tokens.shape[0] % 16 == 0
        and (tokens.shape[0] * n_tp) % SPAN == 0
    )
    if fits:
        return fused_device(1, n_sp, n_tp, *args)
    return on_device(*args)


def solution(mesh):
    return jax.shard_map(
        layer,
        mesh=mesh,
        in_specs=(
            P(("grp", "sp", "tp"), None, None),
            P(None, "tp"),
            P(None, "tp"),
            P(None, "tp"),
            P("tp", None),
            P("tp"),
            P(),
        ),
        out_specs=P(("grp", "sp", "tp"), None, None),
        check_vma=False,
    )
```
